32 devices in a mesh: ep: 16 (over z, y, x), tp: 2 (over core).
Axes of the slice: x: 2, y: 2, z: 4, core: 2. Of those that a mesh axis runs over, the one named last changes fastest.
Arguments:
- hidden_in: bfloat16 [512, 2048], P('ep'), may hold values from -6 to 6
- past_lengths: int32 [512], P('ep'), may hold values from 1 to 1023, as said below
- key_cache: bfloat16 [512, 1024, 256], P('ep', None, 'tp'), may hold values from -512 to 512
- value_cache: bfloat16 [512, 1024, 256], P('ep', None, 'tp'), may hold values from -6 to 6
- attn_gain: float32 [2048], replicated, may hold values from 0.1 to 1.9
- w_query: bfloat16 [2048, 2048], P(None, 'tp'), may hold values from -0.125 to 0.125
- w_key: bfloat16 [2048, 256], P(None, 'tp'), may hold values from -0.125 to 0.125
- w_value: bfloat16 [2048, 256], P(None, 'tp'), may hold values from -0.125 to 0.125
- lambdas: float32 [16], P('tp'), may hold values from 0.3 to 0.8
- head_gain: float32 [128], replicated, may hold values from 0.1 to 1.9
- w_out: bfloat16 [2048, 2048], P('tp'), may hold values from -0.125 to 0.125
- ffn_gain: float32 [2048], replicated, may hold values from 0.1 to 1.9
- route_ids: int32 [512, 2], P('ep'), may hold values from 0 to 7, all different within a row; in each aligned block of 32 rows (0 to 31, 32 to 63, ...) at most 16 rows name the same one
- route_weights: float32 [512, 2], P('ep'), may hold values from 0.2 to 1
- expert_gate: bfloat16 [16, 2048, 704], P('ep', None, 'tp'), may hold values from -0.125 to 0.125
- expert_up: bfloat16 [16, 2048, 704], P('ep', None, 'tp'), may hold values from -0.125 to 0.125
- expert_down: bfloat16 [16, 704, 2048], P('ep', None, 'tp'), may hold values from -1.25 to 1.25
- gate_vector: bfloat16 [2048], replicated, may hold values from -0.125 to 0.125
- dense_gate: bfloat16 [2048, 5632], P(None, ('ep', 'tp')), may hold values from -0.125 to 0.125
- dense_up: bfloat16 [2048, 5632], P(None, ('ep', 'tp')), may hold values from -0.125 to 0.125
- dense_down: bfloat16 [5632, 2048], P('ep', 'tp'), may hold values from -0.625 to 0.625
Outputs:
- mixed_out: bfloat16 [512, 2048], P('ep', 'tp')
- new_keys: bfloat16 [512, 256], P('ep', 'tp')
- new_values: bfloat16 [512, 256], P('ep', 'tp')
The draws below stay inside these ranges and needn't reach their ends.
Inputs may be any that keep to these rules, and one draw needn't show every extreme that they name: `past_lengths`: the new token of a sequence stands at this position; some sequence has 1023 cached positions in every draw. `route_ids`: each row names 2 different experts; among the rows of one index of ep no expert is named more than 16 times, a bound that some block reaches in every draw.
All inputs are finite; a program needn't handle non-finite values.
Results may differ from the reference program's by a relative error of at most 0.02.
The reference program's roundings to bfloat16 on the way count: a program that leaves them out, or rounds other values in their place, can miss the bound.
Values may be sent and summed in bfloat16 or wider, within the bound.
A program may use at most 128 MiB of HBM per device.

```python
import math
import jax
import jax.numpy as jnp
import numpy as np
from jax import lax

D = 2048
HEADS = 16
KV_HEADS = 2
HEAD_DIM = 64
VALUE_DIM = 128
EXPERT_W = 1408
FF_DENSE = 5632
TOP = 2
CACHE_LEN = 1024
SEQ_GRP = 32
EXPERTS = 8
CAP = 16
SEQS = 512
N_EP = 16
N_TP = 2


def draw_past_lengths(key, part):
    key_top, key_share, key_pick = jax.random.split(jax.random.fold_in(key, 71), 3)
    groups = SEQS // SEQ_GRP
    reach_top = jax.random.randint(key_top, (groups, 1), CACHE_LEN // 8, CACHE_LEN)
    shares = jax.random.randint(key_share, (groups, SEQ_GRP), 0, 65536)
    lengths = (1 + (reach_top - 1) * shares // 65536).reshape(-1)
    chosen = jax.random.randint(key_pick, (), 0, SEQS)
    return jnp.where(jnp.arange(SEQS) == chosen, CACHE_LEN - 1, lengths).astype(jnp.int32)


def draw_key_cache(key, part):
    key_drawn = jax.random.fold_in(jax.random.fold_in(key, 73), 0)
    extent = (SEQS, CACHE_LEN, KV_HEADS * 2 * HEAD_DIM)
    drawn_keys = jax.random.truncated_normal(key_drawn, -4.0, 4.0, extent, jnp.float32) * 1.7
    return drawn_keys.astype(jnp.bfloat16)


def shard_levels(own_key, dims, cuts, least, high):
    loudness = 1.0
    for dim, blocks in cuts:
        draws = jax.random.uniform(jax.random.fold_in(jax.random.fold_in(own_key, 6), dim), (blocks,), jnp.float32, least / len(cuts), high / len(cuts))
        loudness = loudness * jnp.repeat(jnp.exp(draws), dims[dim] // blocks).reshape((-1,) + (1,) * (len(dims) - 1 - dim))
    return loudness


def routed_block(stream_key, own, number, rows, number_of, top, limit, slope):
    sequence = jax.random.permutation(stream_key, number_of)
    crowded, usual = portions_of(number_of, rows * top, limit, slope, True), portions_of(number_of, rows * top, limit, slope, False)
    places = jnp.arange(number_of)

    def named(sizes, turn):
        used = int((sizes > 0).sum())
        fixed = max(1, used // 4)
        moved = fixed + (places - fixed + turn * (used - fixed)) % max(1, number_of - fixed)
        return jnp.zeros((number_of,), jnp.int32).at[sequence[jnp.where(places < fixed, places, moved)]].set(jnp.asarray(sizes, jnp.int32))

    sizes = jnp.where(number % 4 == 0, named(crowded, number // 4), named(usual, number - number // 4 - 1))
    mixed = jax.random.permutation(jax.random.fold_in(own, 3), number_of)
    giver, sink = mixed[0:number_of // 2 * 2:2], mixed[1:number_of // 2 * 2:2]
    room = jnp.minimum(sizes[giver] - 1, limit - sizes[sink]) // 2
    room = jnp.where((giver == sequence[0]) | (sink == sequence[0]) | (sizes[sink] == 0), 0, jnp.maximum(room, 0))
    moved = jax.random.randint(jax.random.fold_in(own, 4), (number_of // 2,), 0, 1 << 20) % (room + 1)
    sizes = sizes.at[giver].add(-moved).at[sink].add(moved)
    items = jnp.searchsorted(jnp.cumsum(sizes), jnp.arange(rows * top), side="right").astype(jnp.int32)
    grid = items.reshape(top, rows).T
    grid = grid[jax.random.permutation(jax.random.fold_in(own, 1), rows)]
    turn = jax.random.randint(jax.random.fold_in(own, 2), (rows, 1), 0, top)
    return jnp.take_along_axis(grid, (jnp.arange(top)[None, :] + turn) % top, axis=1)


def portions_of(amount, total, limit, slope, full):
    loads = [(1 << 20) // math.isqrt(rank ** slope) + 1 for rank in range(1, amount + 1)]
    largest = limit if full else min(limit, max(-(-total // amount), total * loads[0] // sum(loads)))
    least = 1 if total - largest >= amount - 1 else 0
    given, spare = [largest] + [least] * (amount - 1), total - largest - least * (amount - 1)
    while spare > 0:
        movable = [i for i in range(1, amount) if given[i] < largest] or [i for i in range(1, amount) if given[i] < limit]
        pool, left = sum([loads[i] for i in movable]), spare
        for i in movable:
            addition = min(limit - given[i], max(1, left * loads[i] // pool), spare)
            given[i] = given[i] + addition
            spare = spare - addition
    return np.array(given)


def noise(own_key, shape, spread, bound, pieces=(), held_as=jnp.bfloat16):
    gain = shard_levels(own_key, shape, pieces, -0.22, 0.18) if pieces else 1.0
    values = jax.random.normal(own_key, shape, jnp.float32) * spread * gain
    return jnp.minimum(jnp.maximum(values, -bound), bound).astype(held_as)


def setup_inputs(seed: int = 0) -> dict:
    key_of = jax.random.split(jax.random.key(seed), 22)
    hidden_in = noise(key_of[0], (SEQS, D), 1.0, 6.0, ((0, 16),))
    past_lengths = draw_past_lengths(jax.random.fold_in(key_of[21], 71), 0)
    key_cache = draw_key_cache(jax.random.fold_in(key_of[21], 71), 0)
    value_cache = noise(key_of[3], (SEQS, CACHE_LEN, KV_HEADS * VALUE_DIM), 1.0, 6.0, ((0, 16), (2, 2)))
    attn_gain = jnp.clip(1.0 + 0.18 * jax.random.normal(key_of[4], (D,), jnp.float32), 0.1, 1.9)
    w_query = noise(key_of[5], (D, HEADS * 2 * HEAD_DIM), D ** -0.5, 0.125, ((1, 2),))
    w_key = noise(key_of[6], (D, KV_HEADS * 2 * HEAD_DIM), D ** -0.5, 0.125, ((1, 2),))
    w_value = noise(key_of[7], (D, KV_HEADS * VALUE_DIM), D ** -0.5, 0.125, ((1, 2),))
    lambdas = jnp.clip(0.3 + 0.5 * jax.random.uniform(key_of[8], (HEADS,), jnp.float32) ** shard_levels(key_of[8], (HEADS,), ((0, 2),), -0.2, 0.2), 0.3, 0.8)
    head_gain = jnp.clip(1.0 + 0.18 * jax.random.normal(key_of[9], (VALUE_DIM,), jnp.float32), 0.1, 1.9)
    w_out = noise(key_of[10], (HEADS * VALUE_DIM, D), (HEADS * VALUE_DIM) ** -0.5, 0.125, ((0, 2),))
    ffn_gain = jnp.clip(1.0 + 0.18 * jax.random.normal(key_of[11], (D,), jnp.float32), 0.1, 1.9)
    route_ids_keys = jax.random.split(jax.random.fold_in(key_of[12], 1), SEQS // SEQ_GRP)
    route_ids_turns = jax.random.permutation(jax.random.fold_in(key_of[12], 3), SEQS // SEQ_GRP)
    route_ids = jax.vmap(lambda own, number: routed_block(jax.random.fold_in(key_of[12], 2), own, number, SEQ_GRP, EXPERTS, TOP, CAP, 2))(route_ids_keys, route_ids_turns).reshape((SEQS, TOP))
    route_weights = jnp.clip(0.2 + 0.8 * jax.random.uniform(key_of[13], (SEQS, TOP), jnp.float32) ** shard_levels(key_of[13], (SEQS, TOP), ((0, 16),), -0.2, 0.2), 0.2, 1.0)
    expert_gate = noise(key_of[14], (2 * EXPERTS, D, EXPERT_W // 2), D ** -0.5, 0.125, ((0, 16), (2, 2)))
    expert_up = noise(key_of[15], (2 * EXPERTS, D, EXPERT_W // 2), D ** -0.5, 0.125, ((0, 16), (2, 2)))
    expert_down = noise(key_of[16], (2 * EXPERTS, EXPERT_W // 2, D), (3.0 * EXPERT_W ** -0.5), 1.25, ((0, 16), (2, 2)))
    gate_vector = noise(key_of[17], (D,), D ** -0.5, 0.125)
    dense_gate = noise(key_of[18], (D, FF_DENSE), D ** -0.5, 0.125, ((1, 32),))
    dense_up = noise(key_of[19], (D, FF_DENSE), D ** -0.5, 0.125, ((1, 32),))
    dense_down = noise(key_of[20], (FF_DENSE, D), (3.0 * FF_DENSE ** -0.5), 0.625, ((0, 16), (1, 2)))
    return dict(hidden_in=hidden_in, past_lengths=past_lengths, key_cache=key_cache, value_cache=value_cache, attn_gain=attn_gain, w_query=w_query, w_key=w_key, w_value=w_value, lambdas=lambdas, head_gain=head_gain, w_out=w_out, ffn_gain=ffn_gain, route_ids=route_ids, route_weights=route_weights, expert_gate=expert_gate, expert_up=expert_up, expert_down=expert_down, gate_vector=gate_vector, dense_gate=dense_gate, dense_up=dense_up, dense_down=dense_down)


norm_eps = 1e-05
rope_base = 10000.0

def rms_rows(values, scales):
    values = values.astype(jnp.float32)
    return values * lax.rsqrt(lax.optimization_barrier(jnp.mean(values * values, axis=-1, keepdims=True)) + norm_eps) * scales

def rotary(values, position):
    middle = values.shape[-1] // 2
    inverse = rope_base ** (-jnp.arange(middle, dtype=jnp.float32) / middle)
    angles = position.astype(jnp.float32)[:, None] * inverse[None, :]
    cosine = jnp.cos(angles)[:, None, None, :]
    sine_part = jnp.sin(angles)[:, None, None, :]
    leading, second = (values[..., :middle], values[..., middle:])
    return jnp.concatenate([leading * cosine - second * sine_part, second * cosine + leading * sine_part], axis=-1)

def rounded(values):
    return lax.optimization_barrier(values.astype(jnp.bfloat16)).astype(jnp.float32)

def reference(hidden_in, past_lengths, key_cache, value_cache, attn_gain, w_query, w_key, w_value, lambdas, head_gain, w_out, ffn_gain, route_ids, route_weights, expert_gate, expert_up, expert_down, gate_vector, dense_gate, dense_up, dense_down):
    batch_rows = hidden_in.shape[0]
    normed = rms_rows(hidden_in, attn_gain).astype(jnp.bfloat16)
    queries = rotary(jnp.dot(normed, w_query, preferred_element_type=jnp.float32).reshape(batch_rows, HEADS, 2, HEAD_DIM), past_lengths).astype(jnp.bfloat16)
    key_new = rotary(jnp.dot(normed, w_key, preferred_element_type=jnp.float32).reshape(batch_rows, KV_HEADS, 2, HEAD_DIM), past_lengths).astype(jnp.bfloat16)
    value_new = jnp.dot(normed, w_value, preferred_element_type=jnp.float32).astype(jnp.bfloat16)
    per_key = HEADS // KV_HEADS
    scale_qk = HEAD_DIM ** (-0.5)

    def attend(packed):
        query_seq, key_seq, value_seq, cache_keys, cache_values, length = packed
        grouped = query_seq.reshape(KV_HEADS, per_key, 2, HEAD_DIM).astype(jnp.float32)
        key_rows = cache_keys.reshape(CACHE_LEN, KV_HEADS, 2, HEAD_DIM).astype(jnp.float32)
        value_rows = cache_values.reshape(CACHE_LEN, KV_HEADS, VALUE_DIM).astype(jnp.float32)
        scores = jnp.einsum('gamd,lgmd->gaml', grouped, key_rows) * scale_qk
        own_score = jnp.einsum('gamd,gmd->gam', grouped, key_seq.astype(jnp.float32)) * scale_qk
        usable = jnp.arange(CACHE_LEN) < length
        scores = jnp.where(usable, scores, -jnp.inf)
        highest = jnp.maximum(lax.optimization_barrier(jnp.max(scores, axis=-1)), own_score)
        weights = jnp.exp(scores - highest[..., None])
        own_weight = jnp.exp(own_score - highest)
        totals = lax.optimization_barrier(jnp.sum(weights, axis=-1)) + own_weight
        summed = jnp.einsum('gaml,lge->game', rounded(weights), value_rows)
        summed = summed + rounded(own_weight)[..., None] * value_seq.reshape(KV_HEADS, 1, 1, VALUE_DIM).astype(jnp.float32)
        return (summed / totals[..., None]).reshape(HEADS, 2, VALUE_DIM)
    mapped = lax.map(attend, (queries, key_new, value_new, key_cache, value_cache, past_lengths))
    head_mix = mapped[:, :, 0] - lambdas[None, :, None] * mapped[:, :, 1]
    head_out = rms_rows(head_mix, head_gain).astype(jnp.bfloat16).reshape(batch_rows, N_TP, -1)
    out_rows = w_out.reshape(N_TP, -1, D)
    partials = jnp.einsum('sgk,gkd->sgd', head_out.astype(jnp.float32), out_rows.astype(jnp.float32))
    attn_out = lax.optimization_barrier(jnp.sum(rounded(partials), axis=1)).astype(jnp.bfloat16)
    residual = hidden_in.astype(jnp.float32) + attn_out.astype(jnp.float32)
    moe_in = rms_rows(residual, ffn_gain).astype(jnp.bfloat16)
    mix_gate = jax.nn.sigmoid(jnp.dot(moe_in, gate_vector, preferred_element_type=jnp.float32)).astype(jnp.bfloat16)
    slot_count = N_EP * CAP
    gate_pairs = expert_gate.reshape(EXPERTS, 2, D, -1)
    up_pairs = expert_up.reshape(EXPERTS, 2, D, -1)
    down_pairs = expert_down.reshape(EXPERTS, 2, -1, D)

    def add_expert(expert, moe_total):
        matches = route_ids == expert
        weight = lax.optimization_barrier(jnp.sum(jnp.where(matches, route_weights, 0.0), axis=1))
        chosen = jnp.any(matches, axis=1)
        number = jnp.sum(chosen.astype(jnp.int32))
        picked = jnp.nonzero(chosen, size=slot_count, fill_value=0)[0]
        live_slot = (jnp.arange(slot_count) < number).astype(jnp.float32)
        taken = moe_in[picked]
        gates_here = lax.dynamic_index_in_dim(gate_pairs, expert, 0, keepdims=False)
        ups_here = lax.dynamic_index_in_dim(up_pairs, expert, 0, keepdims=False)
        downs_here = lax.dynamic_index_in_dim(down_pairs, expert, 0, keepdims=False)
        result = jnp.zeros((slot_count, D), jnp.float32)
        for half_index in range(2):
            gate_pre = jnp.dot(taken, gates_here[half_index], preferred_element_type=jnp.float32)
            up_pre = jnp.dot(taken, ups_here[half_index], preferred_element_type=jnp.float32)
            inner_act = (jax.nn.silu(gate_pre) * up_pre).astype(jnp.bfloat16)
            result = result + jnp.dot(inner_act, downs_here[half_index], preferred_element_type=jnp.float32)
        return moe_total.at[picked].add(result * (weight[picked] * live_slot)[:, None])
    moe_out = lax.fori_loop(0, EXPERTS, add_expert, jnp.zeros((batch_rows, D), jnp.float32))
    dense_pre = jnp.dot(moe_in, dense_gate, preferred_element_type=jnp.float32)
    dense_upper = jnp.dot(moe_in, dense_up, preferred_element_type=jnp.float32)
    dense_act = (jax.nn.silu(dense_pre) * dense_upper).astype(jnp.bfloat16)
    dense_out = jnp.dot(dense_act, dense_down, preferred_element_type=jnp.float32) * mix_gate.astype(jnp.float32)[:, None]
    mixed_out = (residual + moe_out + dense_out).astype(jnp.bfloat16)
    return (mixed_out, key_new.reshape(batch_rows, -1), value_new)
```

```python
import functools

import jax
import jax.numpy as jnp
from jax import lax
from jax.experimental import pallas as pl
from jax.experimental.pallas import tpu as pltpu
from jax.sharding import PartitionSpec as P

HEAD_DIM = 64
VALUE_DIM = 128
EPS = 1e-05
ROPE_BASE = 10000.0
SPAN = 256
GROUP = 4
F32 = jnp.float32
BF16 = jnp.bfloat16
MESH = pl.DeviceIdType.MESH
VMEM = pl.BlockSpec(memory_space=pltpu.VMEM)
ANY = pl.BlockSpec(memory_space=pl.ANY)
SMEM = pl.BlockSpec(memory_space=pltpu.SMEM)


def loop(low, high, body):
    def step(index, carry):
        body(index)
        return carry

    lax.fori_loop(low, high, step, 0)


def attention_kernel(
    lens, hid, cos, sin, again, lam, hgain, wq_any, wk_any, wv_any, wo_any, kc, vc,
    part, kn_out, vn_out,
    wq, wk, wv, wo, kbuf, vbuf, q3, ho3, kn, vn, wsem, csem,
):
    rows = hid.shape[0]
    heads = lam.shape[0]
    spans = kc.shape[1] // SPAN
    groups = rows // GROUP
    loads = [
        pltpu.make_async_copy(src, dst, wsem.at[i])
        for i, (src, dst) in enumerate(((wq_any, wq), (wk_any, wk), (wv_any, wv), (wo_any, wo)))
    ]
    for load in loads[:3]:
        load.start()

    def cache_copies(group, act):
        slot = group % 2
        for i in range(GROUP):
            seq = group * GROUP + i
            need = (lens[seq] + SPAN - 1) // SPAN
            for b in range(spans):
                def both(i=i, seq=seq, b=b):
                    piece = pl.ds(b * SPAN, SPAN)
                    for k, (cache, buf) in enumerate(((kc, kbuf), (vc, vbuf))):
                        act(pltpu.make_async_copy(
                            cache.at[seq, piece, :], buf.at[slot, i, piece, :],
                            csem.at[slot, i, b, k],
                        ))

                pl.when(b < need)(both)

    vbuf[...] = jnp.zeros_like(vbuf)
    cache_copies(0, lambda c: c.start())
    loads[3].start()

    x = hid[...].astype(F32)
    normed = (x * lax.rsqrt(jnp.mean(x * x, axis=-1, keepdims=True) + EPS) * again[...]).astype(BF16)
    lane = lax.broadcasted_iota(jnp.int32, (rows, 128), 1)
    front = (lane % HEAD_DIM) < HEAD_DIM // 2

    def rope(t):
        swapped = jnp.where(front, pltpu.roll(t, 96, 1), pltpu.roll(t, 32, 1))
        return (t * cos[...] + swapped * sin[...]).astype(BF16)

    loads[0].wait()
    for pair in range(heads // 2):
        q = jnp.dot(normed, wq[:, pair * 256:(pair + 1) * 256], preferred_element_type=F32)
        for k in range(2):
            q3[:, pair * 2 + k, :] = rope(q[:, k * 128:(k + 1) * 128]).astype(F32) * (HEAD_DIM ** -0.5)
    loads[1].wait()
    loads[2].wait()
    key = rope(jnp.dot(normed, wk[...], preferred_element_type=F32))
    kn_out[...] = key
    kn[...] = key.astype(F32)
    val = jnp.dot(normed, wv[...], preferred_element_type=F32).astype(BF16)
    vn_out[...] = val
    vn[...] = val.astype(F32)
    lane8 = lax.broadcasted_iota(jnp.int32, (heads, 128), 1)

    def compute(group, width):
        slot = group % 2
        seqs = [group * GROUP + i for i in range(GROUP)]
        owns, scores = [], []
        for i, seq in enumerate(seqs):
            q8 = q3[seq]
            zero = jnp.zeros_like(q8)
            q16 = jnp.concatenate(
                [jnp.where(lane8 < HEAD_DIM, q8, zero), jnp.where(lane8 < HEAD_DIM, zero, q8)], axis=0
            )
            owns.append(jnp.sum(q16 * kn[pl.ds(seq, 1), :], axis=1, keepdims=True))
            scores.append(lax.dot_general(
                q16.astype(BF16), kbuf[slot, i, :width, :], (((1,), (1,)), ((), ())),
                preferred_element_type=F32,
            ))
        place = lax.broadcasted_iota(jnp.int32, scores[0].shape, 1)
        weights, totals, own_weights = [], [], []
        for i, seq in enumerate(seqs):
            s = jnp.where(place < lens[seq], scores[i], -jnp.inf)
            top = jnp.maximum(jnp.max(s, axis=1, keepdims=True), owns[i])
            w = jnp.exp(s - top)
            own = jnp.exp(owns[i] - top)
            totals.append(jnp.sum(w, axis=1, keepdims=True) + own)
            weights.append(w.astype(BF16))
            own_weights.append(own.astype(BF16).astype(F32))
        for i, seq in enumerate(seqs):
            summed = jnp.dot(weights[i], vbuf[slot, i, :width, :], preferred_element_type=F32)
            mapped = (summed + own_weights[i] * vn[pl.ds(seq, 1), :]) / totals[i]
            mix = mapped[:heads] - lam[...] * mapped[heads:]
            ho3[seq] = mix * lax.rsqrt(jnp.mean(mix * mix, axis=-1, keepdims=True) + EPS) * hgain[...]

    def visit(group):
        @pl.when(group + 1 < groups)
        def _():
            cache_copies(group + 1, lambda c: c.start())

        cache_copies(group, lambda c: c.wait())
        longest = lens[group * GROUP]
        for i in range(1, GROUP):
            longest = jnp.maximum(longest, lens[group * GROUP + i])
        need = (longest + SPAN - 1) // SPAN
        for b in range(1, spans + 1):
            pl.when(need == b)(functools.partial(compute, group, b * SPAN))

    loop(0, groups, visit)
    ho = jnp.concatenate([ho3[:, a, :] for a in range(heads)], axis=1).astype(BF16)
    loads[3].wait()
    width = wo.shape[1]
    for t in range(width // 512):
        cols = slice(t * 512, (t + 1) * 512)
        part[:, cols] = jnp.dot(ho, wo[:, cols], preferred_element_type=F32).astype(BF16)


def ffn_kernel(
    n, zs,
    part, hid, fgain, wt, gvec, eg_any, eu_any, ed_any, dg_any, du_any, dd_any,
    out,
    eg, eu, ed, dg, du, dd, peer, res, rows, wtb, eact, dact, sp, rp, zsend, zrecv, own,
    wsem, psem, rsend, rrecv, zs_send, pl_send, arr, fw_send, fw_recv, as_send, as_recv,
    sp_send, rp_recv, zq_send, zq_recv,
):
    ms = n // zs
    batch = hid.shape[0]
    half = hid.shape[1] // 2
    me = lax.axis_index("ep")
    c = lax.axis_index("tp")
    z, p = me // ms, me % ms
    other = (me, 1 - c)

    loads = [
        pltpu.make_async_copy(src, dst, wsem.at[i])
        for i, (src, dst) in enumerate((
            (eg_any.at[0], eg), (eu_any.at[0], eu), (dg_any, dg), (du_any, du),
            (ed_any.at[0], ed), (dd_any, dd),
        ))
    ]
    for load in loads:
        load.start()

    barrier = pltpu.get_barrier_semaphore()

    def greet(k):
        pl.semaphore_signal(barrier, inc=1, device_id=((me + k) % n, c), device_id_type=MESH)

    pl.semaphore_signal(barrier, inc=1, device_id=other, device_id_type=MESH)
    loop(1, n, greet)
    pl.semaphore_wait(barrier, n)

    def remote(src, dst, send, recv, where):
        return pltpu.make_async_remote_copy(
            src_ref=src, dst_ref=dst, send_sem=send, recv_sem=recv,
            device_id=where, device_id_type=MESH,
        )

    swap = remote(part, peer, psem.at[0], psem.at[1], other)
    swap.start()

    def route(k):
        return remote(wt, wtb.at[me], rsend.at[k], rrecv.at[me], ((me + k) % n, c))

    loop(1, n, lambda k: route(k).start())
    wtb[me] = wt[...]
    swap.wait()
    attn = (part[...].astype(F32) + peer[...].astype(F32)).astype(BF16).astype(F32)
    residual = hid[...].astype(F32) + attn
    res[...] = residual
    moe = (
        residual * lax.rsqrt(jnp.mean(residual * residual, axis=-1, keepdims=True) + EPS) * fgain[...]
    ).astype(BF16)
    rows[0, me] = moe[:, :half]
    rows[1, me] = moe[:, half:]

    def zcopy(d):
        return remote(rows.at[c, me], rows.at[c, me], zs_send.at[d], arr.at[me], (((z + d) % zs) * ms + p, c))

    def plane(d, k):
        slot = ((z + d) % zs) * ms + p
        return remote(
            rows.at[c, slot], rows.at[c, slot], pl_send.at[d, k], arr.at[slot], (z * ms + (p + k) % ms, c)
        )

    def forward(slot):
        return remote(rows.at[c, slot], rows.at[c, slot], fw_send.at[slot], fw_recv.at[slot], other)

    def arrival(slot):
        return remote(rows.at[c, slot], rows.at[c, slot], fw_send.at[slot], arr.at[slot], other)

    def partner_arrival(slot):
        return remote(rows.at[1 - c, slot], rows.at[1 - c, slot], fw_send.at[slot], fw_recv.at[slot], other)

    loop(1, zs, lambda d: zcopy(d).start())
    loop(1, ms, lambda k: plane(0, k).start())

    def relay(d):
        slot = ((z + d) % zs) * ms + p
        arrival(slot).wait_recv()
        loop(1, ms, lambda k: plane(d, k).start())
        forward(slot).start()

    loop(1, zs, relay)
    for load in loads:
        load.wait()

    def acts(d, buf, k):
        zd = (z + d) % zs
        return remote(buf.at[c, zd], buf.at[c, zd], as_send.at[k, zd], as_recv.at[k, zd], other)

    def first(d):
        zd = (z + d) % zs

        def take(k):
            slot = zd * ms + (p + k) % ms
            arrival(slot).wait_recv()
            forward(slot).start()

        loop(1, ms, take)

        def met(k):
            slot = zd * ms + (p + k) % ms

            @pl.when(slot != me)
            def _():
                partner_arrival(slot).wait_recv()

        loop(0, ms, met)
        block = pl.ds(zd * ms, ms)
        left = rows[0, block].reshape(ms * batch, half)
        right = rows[1, block].reshape(ms * batch, half)

        def both(w):
            return jnp.dot(left, w[:half, :], preferred_element_type=F32) + jnp.dot(
                right, w[half:, :], preferred_element_type=F32
            )

        for buf, gate, up in ((eact, eg, eu), (dact, dg, du)):
            g = both(gate)
            buf[c, zd] = (g / (1.0 + jnp.exp(-g)) * both(up)).astype(BF16)
        acts(d, eact, 0).start()
        acts(d, dact, 1).start()

    loop(0, zs, first)
    loop(1, n, lambda k: remote(
        wt, wtb.at[(me + k) % n], rsend.at[k], rrecv.at[(me + k) % n], other).wait_recv())
    expert = me // 2
    lane = lax.broadcasted_iota(jnp.int32, (batch, 128), 1)
    line = lax.broadcasted_iota(jnp.int32, (batch, 128), 0)

    def send_part(zd, k):
        q = (p + k) % ms
        return remote(sp.at[zd, q], rp.at[zd, p], sp_send.at[zd, k], rp_recv.at[zd, p], (z * ms + q, c))

    def part_arrival(zd, k):
        q = (p + k) % ms
        return remote(sp.at[zd, q], rp.at[zd, q], sp_send.at[zd, k], rp_recv.at[zd, q], (z * ms + q, c))

    def second(i):
        d = (i + 1) % zs
        zd = (z + d) % zs
        for k, buf in enumerate((eact, dact)):
            remote(buf.at[1 - c, zd], buf.at[1 - c, zd], as_send.at[k, zd], as_recv.at[k, zd], other).wait_recv()
        block = pl.ds(zd * ms, ms)
        gate = (
            jnp.sum(rows[0, block].reshape(ms * batch, half).astype(F32) * gvec[:, :half], axis=1, keepdims=True)
            + jnp.sum(rows[1, block].reshape(ms * batch, half).astype(F32) * gvec[:, half:], axis=1, keepdims=True)
        )
        gate = (1.0 / (1.0 + jnp.exp(-gate))).astype(BF16).astype(F32)
        share = jnp.concatenate([
            jnp.sum(jnp.where(lane == line, wtb[zd * ms + q, pl.ds(expert, 1), :], 0.0), axis=1, keepdims=True)
            for q in range(ms)
        ], axis=0)
        ew, dw = eact.shape[-1], dact.shape[-1]
        y = share * (
            jnp.dot(eact[0, zd], ed[:ew, :], preferred_element_type=F32)
            + jnp.dot(eact[1, zd], ed[ew:, :], preferred_element_type=F32)
        ) + gate * (
            jnp.dot(dact[0, zd], dd[:dw, :], preferred_element_type=F32)
            + jnp.dot(dact[1, zd], dd[dw:, :], preferred_element_type=F32)
        )
        sp[zd] = y.astype(BF16).reshape(ms, batch, half)
        loop(1, ms, lambda k: send_part(zd, k).start())

    loop(0, zs, second)

    def gathered(zd):
        loop(1, ms, lambda k: part_arrival(zd, k).wait_recv())
        total = sp[zd, p].astype(F32)
        for k in range(1, ms):
            total = total + rp[zd, (p + k) % ms].astype(F32)
        return total

    def zback(d):
        zd = (z + d) % zs
        return remote(zsend.at[zd], zrecv.at[z], zq_send.at[d], zq_recv.at[z], (zd * ms + p, c))

    def third(d):
        zd = (z + d) % zs
        zsend[zd] = gathered(zd).astype(BF16)
        zback(d).start()

    loop(1, zs, third)
    own[...] = gathered(z) + res[:, pl.ds(pl.multiple_of(c * half, half), half)]

    def last(d):
        zd = (z + d) % zs
        remote(zsend.at[zd], zrecv.at[zd], zq_send.at[d], zq_recv.at[zd], other).wait_recv()
        own[...] += zrecv[zd].astype(F32)

    loop(1, zs, last)
    out[...] = own[...].astype(BF16)

    loop(1, n, lambda k: route(k).wait_send())
    loop(1, zs, lambda d: zcopy(d).wait_send())

    def settle(d):
        loop(1, ms, lambda k: plane(d, k).wait_send())
        acts(d, eact, 0).wait_send()
        acts(d, dact, 1).wait_send()
        zd = (z + d) % zs
        loop(1, ms, lambda k: send_part(zd, k).wait_send())

    loop(0, zs, settle)
    loop(1, n, lambda k: forward((me + k) % n).wait_send())
    loop(1, zs, lambda d: zback(d).wait_send())


def per_device(
    n_ep, hidden_in, past_lengths, key_cache, value_cache, attn_gain, w_query, w_key, w_value, lambdas,
    head_gain, w_out, ffn_gain, route_ids, route_weights, expert_gate, expert_up, expert_down,
    gate_vector, dense_gate, dense_up, dense_down,
):
    batch, width = hidden_in.shape
    half = width // 2
    heads = lambdas.shape[0]
    cache_len = key_cache.shape[1]
    middle = HEAD_DIM // 2
    inverse = ROPE_BASE ** (-jnp.arange(middle, dtype=F32) / middle)
    angles = past_lengths.astype(F32)[:, None] * inverse[None, :]
    cosine, sine = jnp.cos(angles), jnp.sin(angles)
    cos = jnp.concatenate([cosine] * 4, axis=1)
    sin = jnp.concatenate([-sine, sine] * 2, axis=1)
    sem = pltpu.SemaphoreType.DMA
    part, key_new, value_new = pl.pallas_call(
        attention_kernel,
        out_shape=(
            jax.ShapeDtypeStruct((batch, width), BF16),
            jax.ShapeDtypeStruct((batch, 128), BF16),
            jax.ShapeDtypeStruct((batch, 128), BF16),
        ),
        in_specs=[SMEM] + [VMEM] * 6 + [ANY] * 6,
        out_specs=(VMEM, VMEM, VMEM),
        scratch_shapes=[
            pltpu.VMEM(w_query.shape, BF16),
            pltpu.VMEM(w_key.shape, BF16),
            pltpu.VMEM(w_value.shape, BF16),
            pltpu.VMEM(w_out.shape, BF16),
            pltpu.VMEM((2, GROUP, cache_len, 128), BF16),
            pltpu.VMEM((2, GROUP, cache_len, 128), BF16),
            pltpu.VMEM((batch, heads, 128), F32),
            pltpu.VMEM((batch, heads, 128), F32),
            pltpu.VMEM((batch, 128), F32),
            pltpu.VMEM((batch, 128), F32),
            sem((4,)),
            sem((2, GROUP, cache_len // SPAN, 2)),
        ],
        name="attend",
    )(
        past_lengths, hidden_in, cos, sin, attn_gain.reshape(1, -1), lambdas.reshape(-1, 1),
        head_gain.reshape(1, -1), w_query, w_key, w_value, w_out, key_cache, value_cache,
    )
    experts = n_ep // 2
    named = route_ids.T[None, :, :] == jnp.arange(experts)[:, None, None]
    table = jnp.sum(jnp.where(named, route_weights.T[None, :, :], 0.0), axis=1)
    table = jnp.pad(table, ((0, 0), (0, 128 - batch)))
    zs = 4 if n_ep % 4 == 0 else 1
    ms = n_ep // zs
    expert_w, dense_w = expert_gate.shape[2], dense_gate.shape[1]
    mixed = pl.pallas_call(
        functools.partial(ffn_kernel, n_ep, zs),
        out_shape=jax.ShapeDtypeStruct((batch, half), BF16),
        in_specs=[VMEM] * 5 + [ANY] * 6,
        out_specs=VMEM,
        scratch_shapes=[
            pltpu.VMEM(expert_gate.shape[1:], BF16),
            pltpu.VMEM(expert_up.shape[1:], BF16),
            pltpu.VMEM(expert_down.shape[1:], BF16),
            pltpu.VMEM(dense_gate.shape, BF16),
            pltpu.VMEM(dense_up.shape, BF16),
            pltpu.VMEM(dense_down.shape, BF16),
            pltpu.VMEM((batch, width), BF16),
            pltpu.VMEM((batch, width), F32),
            pltpu.VMEM((2, n_ep, batch, half), BF16),
            pltpu.VMEM((n_ep, experts, 128), F32),
            pltpu.VMEM((2, zs, ms * batch, expert_w), BF16),
            pltpu.VMEM((2, zs, ms * batch, dense_w), BF16),
            pltpu.VMEM((zs, ms, batch, half), BF16),
            pltpu.VMEM((zs, ms, batch, half), BF16),
            pltpu.VMEM((zs, batch, half), BF16),
            pltpu.VMEM((zs, batch, half), BF16),
            pltpu.VMEM((batch, half), F32),
            sem((6,)), sem((2,)), sem((n_ep,)), sem((n_ep,)), sem((zs,)), sem((zs, ms)), sem((n_ep,)),
            sem((n_ep,)), sem((n_ep,)), sem((2, zs)), sem((2, zs)), sem((zs, ms)), sem((zs, ms)),
            sem((zs,)), sem((zs,)),
        ],
        compiler_params=pltpu.CompilerParams(collective_id=0, has_side_effects=True),
        name="feed",
    )(
        part, hidden_in, ffn_gain.reshape(1, -1), table, gate_vector.astype(F32).reshape(1, -1),
        expert_gate, expert_up, expert_down, dense_gate, dense_up, dense_down,
    )
    return mixed, key_new, value_new


def solution(mesh):
    return jax.shard_map(
        functools.partial(per_device, mesh.shape["ep"]),
        mesh=mesh,
        in_specs=(
            P("ep", None),
            P("ep"),
            P("ep", None, "tp"),
            P("ep", None, "tp"),
            P(),
            P(None, "tp"),
            P(None, "tp"),
            P(None, "tp"),
            P("tp"),
            P(),
            P("tp", None),
            P(),
            P("ep", None),
            P("ep", None),
            P("ep", None, "tp"),
            P("ep", None, "tp"),
            P("ep", None, "tp"),
            P(),
            P(None, ("ep", "tp")),
            P(None, ("ep", "tp")),
            P("ep", "tp"),
        ),
        out_specs=(P("ep", "tp"), P("ep", "tp"), P("ep", "tp")),
        check_vma=False,
    )
```

```python
import functools

import jax
import jax.numpy as jnp
import numpy as np
from jax import lax
from jax.experimental import pallas as pl
from jax.experimental.pallas import tpu as pltpu
from jax.sharding import PartitionSpec as P

HEAD_DIM = 64
VALUE_DIM = 128
EPS = 1e-05
ROPE_BASE = 10000.0
SPAN = 256
GROUP = 4
F32 = jnp.float32
BF16 = jnp.bfloat16
MESH = pl.DeviceIdType.MESH
VMEM = pl.BlockSpec(memory_space=pltpu.VMEM)
ANY = pl.BlockSpec(memory_space=pl.ANY)
SMEM = pl.BlockSpec(memory_space=pltpu.SMEM)


def loop(low, high, body):
    def step(index, carry):
        body(index)
        return carry

    lax.fori_loop(low, high, step, 0)


def column(row, count):
    spread = (count, row.shape[1])
    lane = lax.broadcasted_iota(jnp.int32, spread, 1)
    line = lax.broadcasted_iota(jnp.int32, spread, 0)
    return jnp.sum(jnp.where(lane == line, row.astype(F32), 0.0), axis=1, keepdims=True)


def attention_kernel(
    lens, lam, lens_row, inverse, hid, again, hgain, wq_any, wk_any, wv_any, wo_any, kc, vc,
    part, kn_out, vn_out,
    wq, wk, wv, wo, kbuf, vbuf, q3, ho3, kn, vn, wsem, csem,
):
    rows = hid.shape[0]
    heads = lam.shape[0]
    spans = kc.shape[1] // SPAN
    groups = rows // GROUP
    loads = [
        pltpu.make_async_copy(src, dst, wsem.at[i])
        for i, (src, dst) in enumerate(((wq_any, wq), (wk_any, wk), (wv_any, wv), (wo_any, wo)))
    ]
    for load in loads[:3]:
        load.start()

    def cache_copies(group, act):
        slot = group % 2
        for i in range(GROUP):
            seq = group * GROUP + i
            need = (lens[seq] + SPAN - 1) // SPAN
            for b in range(spans):
                def both(i=i, seq=seq, b=b):
                    piece = pl.ds(b * SPAN, SPAN)
                    for k, (cache, buf) in enumerate(((kc, kbuf), (vc, vbuf))):
                        act(pltpu.make_async_copy(
                            cache.at[seq, piece, :], buf.at[slot, i, piece, :],
                            csem.at[slot, i, b, k],
                        ))

                pl.when(b < need)(both)

    vbuf[...] = jnp.zeros_like(vbuf)
    cache_copies(0, lambda c: c.start())
    loads[3].start()

    x = hid[...].astype(F32)
    normed = (x * lax.rsqrt(jnp.mean(x * x, axis=-1, keepdims=True) + EPS) * again[...]).astype(BF16)
    lane = lax.broadcasted_iota(jnp.int32, (rows, 128), 1)
    front = (lane % HEAD_DIM) < HEAD_DIM // 2

    angles = column(lens_row[...], rows) * inverse[...]
    cos, sin = jnp.cos(angles), jnp.sin(angles)
    sin = jnp.where(front, -sin, sin)

    def rope(t):
        swapped = jnp.where(front, pltpu.roll(t, 96, 1), pltpu.roll(t, 32, 1))
        return (t * cos + swapped * sin).astype(BF16)

    loads[0].wait()
    for pair in range(heads // 2):
        q = jnp.dot(normed, wq[:, pair * 256:(pair + 1) * 256], preferred_element_type=F32)
        for k in range(2):
            q3[:, pair * 2 + k, :] = rope(q[:, k * 128:(k + 1) * 128]).astype(F32) * (HEAD_DIM ** -0.5)
    loads[1].wait()
    loads[2].wait()
    key = rope(jnp.dot(normed, wk[...], preferred_element_type=F32))
    kn_out[...] = key
    kn[...] = key.astype(F32)
    val = jnp.dot(normed, wv[...], preferred_element_type=F32).astype(BF16)
    vn_out[...] = val
    vn[...] = val.astype(F32)
    lane8 = lax.broadcasted_iota(jnp.int32, (heads, 128), 1)
    line8 = lax.broadcasted_iota(jnp.int32, (heads, 128), 0)
    lam8 = jnp.zeros((heads, 128), F32)
    for a in range(heads):
        lam8 = jnp.where(line8 == a, lam[a], lam8)

    def compute(group, width):
        slot = group % 2
        seqs = [group * GROUP + i for i in range(GROUP)]
        owns, scores = [], []
        for i, seq in enumerate(seqs):
            q8 = q3[seq]
            zero = jnp.zeros_like(q8)
            q16 = jnp.concatenate(
                [jnp.where(lane8 < HEAD_DIM, q8, zero), jnp.where(lane8 < HEAD_DIM, zero, q8)], axis=0
            )
            owns.append(jnp.sum(q16 * kn[pl.ds(seq, 1), :], axis=1, keepdims=True))
            scores.append(lax.dot_general(
                q16.astype(BF16), kbuf[slot, i, :width, :], (((1,), (1,)), ((), ())),
                preferred_element_type=F32,
            ))
        place = lax.broadcasted_iota(jnp.int32, scores[0].shape, 1)
        weights, totals, own_weights = [], [], []
        for i, seq in enumerate(seqs):
            s = jnp.where(place < lens[seq], scores[i], -jnp.inf)
            top = jnp.maximum(jnp.max(s, axis=1, keepdims=True), owns[i])
            w = jnp.exp(s - top)
            own = jnp.exp(owns[i] - top)
            totals.append(jnp.sum(w, axis=1, keepdims=True) + own)
            weights.append(w.astype(BF16))
            own_weights.append(own.astype(BF16).astype(F32))
        for i, seq in enumerate(seqs):
            summed = jnp.dot(weights[i], vbuf[slot, i, :width, :], preferred_element_type=F32)
            mapped = (summed + own_weights[i] * vn[pl.ds(seq, 1), :]) / totals[i]
            mix = mapped[:heads] - lam8 * mapped[heads:]
            ho3[seq] = mix * lax.rsqrt(jnp.mean(mix * mix, axis=-1, keepdims=True) + EPS) * hgain[...]

    def visit(group):
        @pl.when(group + 1 < groups)
        def _():
            cache_copies(group + 1, lambda c: c.start())

        cache_copies(group, lambda c: c.wait())
        longest = lens[group * GROUP]
        for i in range(1, GROUP):
            longest = jnp.maximum(longest, lens[group * GROUP + i])
        need = (longest + SPAN - 1) // SPAN
        for b in range(1, spans + 1):
            pl.when(need == b)(functools.partial(compute, group, b * SPAN))

    loop(0, groups, visit)
    ho = jnp.concatenate([ho3[:, a, :] for a in range(heads)], axis=1).astype(BF16)
    loads[3].wait()
    width = wo.shape[1]
    for t in range(width // 512):
        cols = slice(t * 512, (t + 1) * 512)
        part[:, cols] = jnp.dot(ho, wo[:, cols], preferred_element_type=F32).astype(BF16)


def ffn_kernel(
    n, zs,
    part, hid, fgain, ids, shares, gvec, eg_any, eu_any, ed_any, dg_any, du_any, dd_any,
    out,
    eg, eu, ed, dg, du, dd, peer, res, rows, wtb, eact, dact, sp, rp, zsend, zrecv, own,
    wsem, psem, rsend, rrecv, zs_send, pl_send, hop_send, arr, fw_send, fw_recv, as_send, as_recv,
    sp_send, rp_recv, zq_send, zq_recv,
):
    ms = n // zs
    batch = hid.shape[0]
    half = hid.shape[1] // 2
    me = lax.axis_index("ep")
    c = lax.axis_index("tp")
    z, p = me // ms, me % ms
    other = (me, 1 - c)

    loads = [
        pltpu.make_async_copy(src, dst, wsem.at[i])
        for i, (src, dst) in enumerate((
            (eg_any.at[0], eg), (eu_any.at[0], eu), (dg_any, dg), (du_any, du),
            (ed_any.at[0], ed), (dd_any, dd),
        ))
    ]
    for load in loads:
        load.start()

    experts = wtb.shape[1]
    numbers = lax.broadcasted_iota(jnp.int32, (experts, batch), 0)
    table = jnp.zeros((experts, batch), F32)
    for k in range(ids.shape[0]):
        table = table + jnp.where(ids[k:k + 1, :] == numbers, shares[k:k + 1, :], 0.0)
    wtb[me] = jnp.pad(table, ((0, 0), (0, 128 - batch)))
    barrier = pltpu.get_barrier_semaphore()

    quad = ms == 4

    def flip(q, bit):
        return q + bit - 2 * bit * ((q // bit) % 2)

    def greet(k):
        pl.semaphore_signal(barrier, inc=1, device_id=((me + k) % n, c), device_id_type=MESH)

    pl.semaphore_signal(barrier, inc=1, device_id=other, device_id_type=MESH)
    loop(1, n, greet)
    pl.semaphore_wait(barrier, n)

    def remote(src, dst, send, recv, where):
        return pltpu.make_async_remote_copy(
            src_ref=src, dst_ref=dst, send_sem=send, recv_sem=recv,
            device_id=where, device_id_type=MESH,
        )

    swap = remote(part, peer, psem.at[0], psem.at[1], other)
    swap.start()

    def route(k):
        return remote(wtb.at[me], wtb.at[me], rsend.at[k], rrecv.at[me], ((me + k) % n, c))

    loop(1, n, lambda k: route(k).start())
    swap.wait()
    attn = (part[...].astype(F32) + peer[...].astype(F32)).astype(BF16).astype(F32)
    residual = hid[...].astype(F32) + attn
    res[...] = residual
    moe = (
        residual * lax.rsqrt(jnp.mean(residual * residual, axis=-1, keepdims=True) + EPS) * fgain[...]
    ).astype(BF16)
    rows[0, me] = moe[:, :half]
    rows[1, me] = moe[:, half:]

    def zcopy(d):
        return remote(rows.at[c, me], rows.at[c, me], zs_send.at[d], arr.at[me], (((z + d) % zs) * ms + p, c))

    def plane(d, k):
        slot = ((z + d) % zs) * ms + p
        return remote(
            rows.at[c, slot], rows.at[c, slot], pl_send.at[d, k], arr.at[slot], (z * ms + (p + k) % ms, c)
        )

    def plane4(d, bit):
        slot = ((z + d) % zs) * ms + p
        return remote(
            rows.at[c, slot], rows.at[c, slot], pl_send.at[d, bit], arr.at[slot], (z * ms + flip(p, bit), c)
        )

    def forward(slot):
        return remote(rows.at[c, slot], rows.at[c, slot], fw_send.at[slot], fw_recv.at[slot], other)

    def arrival(slot):
        return remote(rows.at[c, slot], rows.at[c, slot], fw_send.at[slot], arr.at[slot], other)

    def partner_arrival(slot):
        return remote(rows.at[1 - c, slot], rows.at[1 - c, slot], fw_send.at[slot], fw_recv.at[slot], other)

    loop(1, zs, lambda d: zcopy(d).start())

    near = 1 + c
    far = 2 - c

    def hop(slot):
        return remote(
            rows.at[c, slot], rows.at[c, slot], hop_send.at[slot // ms], arr.at[slot],
            (z * ms + flip(p, far), c),
        )

    def spread(d):
        slot = ((z + d) % zs) * ms + p

        @pl.when(d > 0)
        def _():
            arrival(slot).wait_recv()

        if quad:
            plane4(d, 1).start()
            plane4(d, 2).start()
        else:
            loop(1, ms, lambda k: plane(d, k).start())

        @pl.when(d > 0)
        def _():
            forward(slot).start()

    def taken(slot):
        arrival(slot).wait_recv()
        forward(slot).start()

    def collect(d):
        base = ((z + d) % zs) * ms
        if quad:
            slot = base + flip(p, near)
            arrival(slot).wait_recv()
            hop(slot).start()
            forward(slot).start()
            taken(base + flip(p, far))
        else:
            loop(1, ms, lambda k: taken(base + (p + k) % ms))

    def acts(d, buf, k):
        zd = (z + d) % zs
        return remote(buf.at[c, zd], buf.at[c, zd], as_send.at[k, zd], as_recv.at[k, zd], other)

    def first(d):
        zd = (z + d) % zs
        if quad:
            taken(zd * ms + 3 - p)

        def met(k):
            slot = zd * ms + (p + k) % ms

            @pl.when(slot != me)
            def _():
                partner_arrival(slot).wait_recv()

        loop(0, ms, met)
        block = pl.ds(zd * ms, ms)
        left = rows[0, block].reshape(ms * batch, half)
        right = rows[1, block].reshape(ms * batch, half)

        def both(w):
            across = (((1,), (1,)), ((), ()))
            return lax.dot_general(left, w[:, :half], across, preferred_element_type=F32) + lax.dot_general(
                right, w[:, half:], across, preferred_element_type=F32
            )

        for buf, gate, up in ((eact, eg, eu), (dact, dg, du)):
            g = both(gate)
            buf[c, zd] = (g / (1.0 + jnp.exp(-g)) * both(up)).astype(BF16)
        acts(d, eact, 0).start()
        acts(d, dact, 1).start()

    spread(0)

    def gather_step(d):
        @pl.when(d + 1 < zs)
        def _():
            spread(d + 1)

        @pl.when(d < zs)
        def _():
            collect(d)

        @pl.when(d == 1)
        def _():
            for load in loads:
                load.wait()

        @pl.when(d > 0)
        def _():
            first(d - 1)

    loop(0, zs + 1, gather_step)
    loop(1, n, lambda k: remote(
        wtb.at[me], wtb.at[(me + k) % n], rsend.at[k], rrecv.at[(me + k) % n], other).wait_recv())
    expert = me // 2

    def send_part(zd, k):
        q = (p + k) % ms
        return remote(sp.at[zd, q], rp.at[zd, p], sp_send.at[zd, k], rp_recv.at[zd, p], (z * ms + q, c))

    def part_arrival(zd, k):
        q = (p + k) % ms
        return remote(sp.at[zd, q], rp.at[zd, q], sp_send.at[zd, k], rp_recv.at[zd, q], (z * ms + q, c))

    def first_leg(zd, k):
        to = flip(p, near)
        return remote(
            sp.at[zd, 3 - p if k == 0 else to], rp.at[zd, k], sp_send.at[zd, k], rp_recv.at[zd, k],
            (z * ms + to, c),
        )

    def next_leg(zd):
        return remote(
            rp.at[zd, 3], rp.at[zd, 2], sp_send.at[zd, 2], rp_recv.at[zd, 2], (z * ms + flip(p, far), c)
        )

    def pass_on(i):
        zd = (z + i + 1) % zs
        first_leg(zd, 0).wait_recv()
        rp[zd, 3] = (sp[zd, flip(p, far)].astype(F32) + rp[zd, 0].astype(F32)).astype(BF16)
        next_leg(zd).start()

    def second(i):
        d = (i + 1) % zs
        zd = (z + d) % zs
        for k, buf in enumerate((eact, dact)):
            remote(buf.at[1 - c, zd], buf.at[1 - c, zd], as_send.at[k, zd], as_recv.at[k, zd], other).wait_recv()
        block = pl.ds(zd * ms, ms)
        gate = (
            jnp.sum(rows[0, block].reshape(ms * batch, half).astype(F32) * gvec[:, :half].astype(F32), axis=1, keepdims=True)
            + jnp.sum(rows[1, block].reshape(ms * batch, half).astype(F32) * gvec[:, half:].astype(F32), axis=1, keepdims=True)
        )
        gate = (1.0 / (1.0 + jnp.exp(-gate))).astype(BF16).astype(F32)
        share = jnp.concatenate([
            column(wtb[zd * ms + q, pl.ds(expert, 1), :], batch) for q in range(ms)
        ], axis=0)
        ew, dw = eact.shape[-1], dact.shape[-1]
        y = share * (
            jnp.dot(eact[0, zd], ed[:ew, :], preferred_element_type=F32)
            + jnp.dot(eact[1, zd], ed[ew:, :], preferred_element_type=F32)
        ) + gate * (
            jnp.dot(dact[0, zd], dd[:dw, :], preferred_element_type=F32)
            + jnp.dot(dact[1, zd], dd[dw:, :], preferred_element_type=F32)
        )
        sp[zd] = y.astype(BF16).reshape(ms, batch, half)
        if quad:
            first_leg(zd, 0).start()
            first_leg(zd, 1).start()
        else:
            loop(1, ms, lambda k: send_part(zd, k).start())

    def gathered(zd):
        if quad:
            first_leg(zd, 1).wait_recv()
            next_leg(zd).wait_recv()
            return sp[zd, p].astype(F32) + rp[zd, 1].astype(F32) + rp[zd, 2].astype(F32)
        loop(1, ms, lambda k: part_arrival(zd, k).wait_recv())
        total = sp[zd, p].astype(F32)
        for k in range(1, ms):
            total = total + rp[zd, (p + k) % ms].astype(F32)
        return total

    def zback(d):
        zd = (z + d) % zs
        return remote(zsend.at[zd], zrecv.at[z], zq_send.at[d], zq_recv.at[z], (zd * ms + p, c))

    def third(d):
        zd = (z + d) % zs
        zsend[zd] = gathered(zd).astype(BF16)
        zback(d).start()

    def reduce_step(i):
        @pl.when(i < zs)
        def _():
            second(i)

        if quad:
            @pl.when((i > 0) & (i <= zs))
            def _():
                pass_on(i - 1)

        @pl.when((i > 1) & (i <= zs))
        def _():
            third(i - 1)

    loop(0, zs + 1, reduce_step)
    own[...] = gathered(z) + res[:, pl.ds(pl.multiple_of(c * half, half), half)]

    def last(d):
        zd = (z + d) % zs
        remote(zsend.at[zd], zrecv.at[zd], zq_send.at[d], zq_recv.at[zd], other).wait_recv()
        own[...] += zrecv[zd].astype(F32)

    loop(1, zs, last)
    out[...] = own[...].astype(BF16)

    loop(1, n, lambda k: route(k).wait_send())
    loop(1, zs, lambda d: zcopy(d).wait_send())

    def settle(d):
        zd = (z + d) % zs
        if quad:
            plane4(d, 1).wait_send()
            plane4(d, 2).wait_send()
            hop(zd * ms + flip(p, near)).wait_send()
            first_leg(zd, 0).wait_send()
            first_leg(zd, 1).wait_send()
            next_leg(zd).wait_send()
        else:
            loop(1, ms, lambda k: plane(d, k).wait_send())
            loop(1, ms, lambda k: send_part(zd, k).wait_send())
        acts(d, eact, 0).wait_send()
        acts(d, dact, 1).wait_send()

    loop(0, zs, settle)
    loop(1, n, lambda k: forward((me + k) % n).wait_send())
    loop(1, zs, lambda d: zback(d).wait_send())


def per_device(
    n_ep, hidden_in, past_lengths, key_cache, value_cache, attn_gain, w_query, w_key, w_value, lambdas,
    head_gain, w_out, ffn_gain, route_ids, route_weights, expert_gate, expert_up, expert_down,
    gate_vector, dense_gate, dense_up, dense_down,
):
    batch, width = hidden_in.shape
    half = width // 2
    heads = lambdas.shape[0]
    cache_len = key_cache.shape[1]
    middle = HEAD_DIM // 2
    powers = ROPE_BASE ** (-np.arange(middle, dtype=np.float32) / np.float32(middle))
    inverse = jnp.asarray(np.tile(powers.astype(np.float32), 128 // middle)[None, :])
    sem = pltpu.SemaphoreType.DMA
    part, key_new, value_new = pl.pallas_call(
        attention_kernel,
        out_shape=(
            jax.ShapeDtypeStruct((batch, width), BF16),
            jax.ShapeDtypeStruct((batch, 128), BF16),
            jax.ShapeDtypeStruct((batch, 128), BF16),
        ),
        in_specs=[SMEM] * 2 + [VMEM] * 5 + [ANY] * 6,
        out_specs=(VMEM, VMEM, VMEM),
        scratch_shapes=[
            pltpu.VMEM(w_query.shape, BF16),
            pltpu.VMEM(w_key.shape, BF16),
            pltpu.VMEM(w_value.shape, BF16),
            pltpu.VMEM(w_out.shape, BF16),
            pltpu.VMEM((2, GROUP, cache_len, 128), BF16),
            pltpu.VMEM((2, GROUP, cache_len, 128), BF16),
            pltpu.VMEM((batch, heads, 128), F32),
            pltpu.VMEM((batch, heads, 128), F32),
            pltpu.VMEM((batch, 128), F32),
            pltpu.VMEM((batch, 128), F32),
            sem((4,)),
            sem((2, GROUP, cache_len // SPAN, 2)),
        ],
        name="attend",
    )(
        past_lengths, lambdas, past_lengths.reshape(1, -1), inverse, hidden_in,
        attn_gain.reshape(1, -1), head_gain.reshape(1, -1), w_query, w_key, w_value, w_out, key_cache, value_cache,
    )
    experts = n_ep // 2
    zs = 4 if n_ep % 4 == 0 else 1
    ms = n_ep // zs
    expert_w, dense_w = expert_gate.shape[2], dense_gate.shape[1]
    mixed = pl.pallas_call(
        functools.partial(ffn_kernel, n_ep, zs),
        out_shape=jax.ShapeDtypeStruct((batch, half), BF16),
        in_specs=[VMEM] * 6 + [ANY] * 6,
        out_specs=VMEM,
        scratch_shapes=[
            pltpu.VMEM((expert_w, width), BF16),
            pltpu.VMEM((expert_w, width), BF16),
            pltpu.VMEM(expert_down.shape[1:], BF16),
            pltpu.VMEM((dense_w, width), BF16),
            pltpu.VMEM((dense_w, width), BF16),
            pltpu.VMEM(dense_down.shape, BF16),
            pltpu.VMEM((batch, width), BF16),
            pltpu.VMEM((batch, width), F32),
            pltpu.VMEM((2, n_ep, batch, half), BF16),
            pltpu.VMEM((n_ep, experts, 128), F32),
            pltpu.VMEM((2, zs, ms * batch, expert_w), BF16),
            pltpu.VMEM((2, zs, ms * batch, dense_w), BF16),
            pltpu.VMEM((zs, ms, batch, half), BF16),
            pltpu.VMEM((zs, ms, batch, half), BF16),
            pltpu.VMEM((zs, batch, half), BF16),
            pltpu.VMEM((zs, batch, half), BF16),
            pltpu.VMEM((batch, half), F32),
            sem((6,)), sem((2,)), sem((n_ep,)), sem((n_ep,)), sem((zs,)), sem((zs, ms)), sem((zs,)), sem((n_ep,)),
            sem((n_ep,)), sem((n_ep,)), sem((2, zs)), sem((2, zs)), sem((zs, ms)), sem((zs, ms)),
            sem((zs,)), sem((zs,)),
        ],
        compiler_params=pltpu.CompilerParams(collective_id=0, has_side_effects=True),
        name="feed",
    )(
        part, hidden_in, ffn_gain.reshape(1, -1), route_ids.T, route_weights.T, gate_vector.reshape(1, -1),
        expert_gate.swapaxes(1, 2), expert_up.swapaxes(1, 2), expert_down,
        dense_gate.T, dense_up.T, dense_down,
    )
    return mixed, key_new, value_new


def solution(mesh):
    return jax.shard_map(
        functools.partial(per_device, mesh.shape["ep"]),
        mesh=mesh,
        in_specs=(
            P("ep", None),
            P("ep"),
            P("ep", None, "tp"),
            P("ep", None, "tp"),
            P(),
            P(None, "tp"),
            P(None, "tp"),
            P(None, "tp"),
            P("tp"),
            P(),
            P("tp", None),
            P(),
            P("ep", None),
            P("ep", None),
            P("ep", None, "tp"),
            P("ep", None, "tp"),
            P("ep", None, "tp"),
            P(),
            P(None, ("ep", "tp")),
            P(None, ("ep", "tp")),
            P("ep", "tp"),
        ),
        out_specs=(P("ep", "tp"), P("ep", "tp"), P("ep", "tp")),
        check_vma=False,
    )
```

```python
import functools

import jax
import jax.numpy as jnp
import numpy as np
from jax import lax
from jax.experimental import pallas as pl
from jax.experimental.pallas import tpu as pltpu
from jax.sharding import PartitionSpec as P

HEAD_DIM = 64
VALUE_DIM = 128
EPS = 1e-05
ROPE_BASE = 10000.0
SPAN = 256
GROUP = 4
F32 = jnp.float32
BF16 = jnp.bfloat16
MESH = pl.DeviceIdType.MESH
VMEM = pl.BlockSpec(memory_space=pltpu.VMEM)
ANY = pl.BlockSpec(memory_space=pl.ANY)
SMEM = pl.BlockSpec(memory_space=pltpu.SMEM)


def loop(low, high, body):
    def step(index, carry):
        body(index)
        return carry

    lax.fori_loop(low, high, step, 0)


def column(row, count):
    spread = (count, row.shape[1])
    lane = lax.broadcasted_iota(jnp.int32, spread, 1)
    line = lax.broadcasted_iota(jnp.int32, spread, 0)
    return jnp.sum(jnp.where(lane == line, row.astype(F32), 0.0), axis=1, keepdims=True)


def attention_kernel(
    lens, lam, lens_row, inverse, hid, again, hgain, wq_any, wk_any, wv_any, wo_any, kc, vc,
    part, kn_out, vn_out,
    wq, wk, wv, wo, kbuf, vbuf, q3, ho3, kn, vn, wsem, csem,
):
    rows = hid.shape[0]
    heads = lam.shape[0]
    spans = kc.shape[1] // SPAN
    groups = rows // GROUP
    loads = [
        pltpu.make_async_copy(src, dst, wsem.at[i])
        for i, (src, dst) in enumerate(((wq_any, wq), (wk_any, wk), (wv_any, wv), (wo_any, wo)))
    ]
    for load in loads[:3]:
        load.start()

    def cache_copies(group, act):
        slot = group % 2
        for i in range(GROUP):
            seq = group * GROUP + i
            need = (lens[seq] + SPAN - 1) // SPAN
            for b in range(spans):
                def both(i=i, seq=seq, b=b):
                    piece = pl.ds(b * SPAN, SPAN)
                    for k, (cache, buf) in enumerate(((kc, kbuf), (vc, vbuf))):
                        act(pltpu.make_async_copy(
                            cache.at[seq, piece, :], buf.at[slot, i, piece, :],
                            csem.at[slot, i, b, k],
                        ))

                pl.when(b < need)(both)

    vbuf[...] = jnp.zeros_like(vbuf)
    cache_copies(0, lambda c: c.start())
    loads[3].start()

    x = hid[...].astype(F32)
    normed = (x * lax.rsqrt(jnp.mean(x * x, axis=-1, keepdims=True) + EPS) * again[...]).astype(BF16)
    lane = lax.broadcasted_iota(jnp.int32, (rows, 128), 1)
    front = (lane % HEAD_DIM) < HEAD_DIM // 2

    angles = column(lens_row[...], rows) * inverse[...]
    cos, sin = jnp.cos(angles), jnp.sin(angles)
    sin = jnp.where(front, -sin, sin)

    def rope(t):
        swapped = jnp.where(front, pltpu.roll(t, 96, 1), pltpu.roll(t, 32, 1))
        return (t * cos + swapped * sin).astype(BF16)

    loads[0].wait()
    for pair in range(heads // 2):
        q = jnp.dot(normed, wq[:, pair * 256:(pair + 1) * 256], preferred_element_type=F32)
        for k in range(2):
            q3[:, pair * 2 + k, :] = rope(q[:, k * 128:(k + 1) * 128]).astype(F32) * (HEAD_DIM ** -0.5)
    loads[1].wait()
    loads[2].wait()
    key = rope(jnp.dot(normed, wk[...], preferred_element_type=F32))
    kn_out[...] = key
    kn[...] = key.astype(F32)
    val = jnp.dot(normed, wv[...], preferred_element_type=F32).astype(BF16)
    vn_out[...] = val
    vn[...] = val.astype(F32)
    lane8 = lax.broadcasted_iota(jnp.int32, (heads, 128), 1)
    line8 = lax.broadcasted_iota(jnp.int32, (heads, 128), 0)
    lam8 = jnp.zeros((heads, 128), F32)
    for a in range(heads):
        lam8 = jnp.where(line8 == a, lam[a], lam8)

    def compute(group, width):
        slot = group % 2
        seqs = [group * GROUP + i for i in range(GROUP)]
        owns, scores = [], []
        for i, seq in enumerate(seqs):
            q8 = q3[seq]
            zero = jnp.zeros_like(q8)
            q16 = jnp.concatenate(
                [jnp.where(lane8 < HEAD_DIM, q8, zero), jnp.where(lane8 < HEAD_DIM, zero, q8)], axis=0
            )
            owns.append(jnp.sum(q16 * kn[pl.ds(seq, 1), :], axis=1, keepdims=True))
            scores.append(lax.dot_general(
                q16.astype(BF16), kbuf[slot, i, :width, :], (((1,), (1,)), ((), ())),
                preferred_element_type=F32,
            ))
        place = lax.broadcasted_iota(jnp.int32, scores[0].shape, 1)
        weights, totals, own_weights = [], [], []
        for i, seq in enumerate(seqs):
            s = jnp.where(place < lens[seq], scores[i], -jnp.inf)
            top = jnp.maximum(jnp.max(s, axis=1, keepdims=True), owns[i])
            w = jnp.exp(s - top)
            own = jnp.exp(owns[i] - top)
            totals.append(jnp.sum(w, axis=1, keepdims=True) + own)
            weights.append(w.astype(BF16))
            own_weights.append(own.astype(BF16).astype(F32))
        for i, seq in enumerate(seqs):
            summed = jnp.dot(weights[i], vbuf[slot, i, :width, :], preferred_element_type=F32)
            mapped = (summed + own_weights[i] * vn[pl.ds(seq, 1), :]) / totals[i]
            mix = mapped[:heads] - lam8 * mapped[heads:]
            ho3[seq] = mix * lax.rsqrt(jnp.mean(mix * mix, axis=-1, keepdims=True) + EPS) * hgain[...]

    def visit(group):
        @pl.when(group + 1 < groups)
        def _():
            cache_copies(group + 1, lambda c: c.start())

        cache_copies(group, lambda c: c.wait())
        longest = lens[group * GROUP]
        for i in range(1, GROUP):
            longest = jnp.maximum(longest, lens[group * GROUP + i])
        need = (longest + SPAN - 1) // SPAN
        for b in range(1, spans + 1):
            pl.when(need == b)(functools.partial(compute, group, b * SPAN))

    loop(0, groups, visit)
    ho = jnp.concatenate([ho3[:, a, :] for a in range(heads)], axis=1).astype(BF16)
    loads[3].wait()
    width = wo.shape[1]
    for t in range(width // 512):
        cols = slice(t * 512, (t + 1) * 512)
        part[:, cols] = jnp.dot(ho, wo[:, cols], preferred_element_type=F32).astype(BF16)


def ffn_kernel(
    n, zs,
    part, hid, fgain, ids, shares, gvec, eg_any, eu_any, ed_any, dg_any, du_any, dd_any,
    out,
    eg, eu, ed, dg, du, dd, peer, res, rows, wtb, eact, dact, sp, rp, zsend, zrecv, own, gline,
    wsem, psem, rsend, rrecv, zs_send, pl_send, hop_send, arr, fw_send, fw_recv, as_send, as_recv,
    sp_send, rp_recv, zq_send, zq_recv,
):
    ms = n // zs
    batch = hid.shape[0]
    half = hid.shape[1] // 2
    me = lax.axis_index("ep")
    c = lax.axis_index("tp")
    z, p = me // ms, me % ms
    other = (me, 1 - c)

    loads = [
        pltpu.make_async_copy(src, dst, wsem.at[i])
        for i, (src, dst) in enumerate((
            (eg_any.at[0], eg), (eu_any.at[0], eu), (dg_any, dg), (du_any, du),
            (ed_any.at[0], ed), (dd_any, dd),
        ))
    ]
    for load in loads:
        load.start()

    experts = wtb.shape[1]
    gates = gvec[...].astype(F32)
    gates = jnp.concatenate([gates[i:i + 1] for i in range(gates.shape[0])], axis=1)
    gline[...] = gates
    numbers = lax.broadcasted_iota(jnp.int32, (experts, batch), 0)
    table = jnp.zeros((experts, batch), F32)
    for k in range(ids.shape[0]):
        table = table + jnp.where(ids[k:k + 1, :] == numbers, shares[k:k + 1, :], 0.0)
    wtb[me] = jnp.pad(table, ((0, 0), (0, 128 - batch)))
    barrier = pltpu.get_barrier_semaphore()

    quad = ms == 4

    def flip(q, bit):
        return q + bit - 2 * bit * ((q // bit) % 2)

    def greet(k):
        pl.semaphore_signal(barrier, inc=1, device_id=((me + k) % n, c), device_id_type=MESH)

    pl.semaphore_signal(barrier, inc=1, device_id=other, device_id_type=MESH)
    loop(1, n, greet)
    pl.semaphore_wait(barrier, n)

    def remote(src, dst, send, recv, where):
        return pltpu.make_async_remote_copy(
            src_ref=src, dst_ref=dst, send_sem=send, recv_sem=recv,
            device_id=where, device_id_type=MESH,
        )

    swap = remote(part, peer, psem.at[0], psem.at[1], other)
    swap.start()

    def route(k):
        return remote(wtb.at[me], wtb.at[me], rsend.at[k], rrecv.at[me], ((me + k) % n, c))

    loop(1, n, lambda k: route(k).start())
    swap.wait()
    attn = (part[...].astype(F32) + peer[...].astype(F32)).astype(BF16).astype(F32)
    residual = hid[...].astype(F32) + attn
    res[...] = residual
    moe = (
        residual * lax.rsqrt(jnp.mean(residual * residual, axis=-1, keepdims=True) + EPS) * fgain[...]
    ).astype(BF16)
    rows[0, me] = moe[:, :half]
    rows[1, me] = moe[:, half:]

    def zcopy(d):
        return remote(rows.at[c, me], rows.at[c, me], zs_send.at[d], arr.at[me], (((z + d) % zs) * ms + p, c))

    def plane(d, k):
        slot = ((z + d) % zs) * ms + p
        return remote(
            rows.at[c, slot], rows.at[c, slot], pl_send.at[d, k], arr.at[slot], (z * ms + (p + k) % ms, c)
        )

    def plane4(d, bit):
        slot = ((z + d) % zs) * ms + p
        return remote(
            rows.at[c, slot], rows.at[c, slot], pl_send.at[d, bit], arr.at[slot], (z * ms + flip(p, bit), c)
        )

    def forward(slot):
        return remote(rows.at[c, slot], rows.at[c, slot], fw_send.at[slot], fw_recv.at[slot], other)

    def arrival(slot):
        return remote(rows.at[c, slot], rows.at[c, slot], fw_send.at[slot], arr.at[slot], other)

    def partner_arrival(slot):
        return remote(rows.at[1 - c, slot], rows.at[1 - c, slot], fw_send.at[slot], fw_recv.at[slot], other)

    loop(1, zs, lambda d: zcopy(d).start())

    near = 1 + c
    far = 2 - c

    def hop(slot):
        return remote(
            rows.at[c, slot], rows.at[c, slot], hop_send.at[slot // ms], arr.at[slot],
            (z * ms + flip(p, far), c),
        )

    def spread(d):
        slot = ((z + d) % zs) * ms + p

        @pl.when(d > 0)
        def _():
            arrival(slot).wait_recv()

        if quad:
            plane4(d, 1).start()
            plane4(d, 2).start()
        else:
            loop(1, ms, lambda k: plane(d, k).start())

        @pl.when(d > 0)
        def _():
            forward(slot).start()

    def taken(slot):
        arrival(slot).wait_recv()
        forward(slot).start()

    def collect(d):
        base = ((z + d) % zs) * ms
        if quad:
            slot = base + flip(p, near)
            arrival(slot).wait_recv()
            hop(slot).start()
            forward(slot).start()
            taken(base + flip(p, far))
        else:
            loop(1, ms, lambda k: taken(base + (p + k) % ms))

    def acts(d, buf, k):
        zd = (z + d) % zs
        return remote(buf.at[c, zd], buf.at[c, zd], as_send.at[k, zd], as_recv.at[k, zd], other)

    def first(d):
        zd = (z + d) % zs
        if quad:
            taken(zd * ms + 3 - p)

        def met(k):
            slot = zd * ms + (p + k) % ms

            @pl.when(slot != me)
            def _():
                partner_arrival(slot).wait_recv()

        loop(0, ms, met)
        block = pl.ds(zd * ms, ms)
        left = rows[0, block].reshape(ms * batch, half)
        right = rows[1, block].reshape(ms * batch, half)

        def both(w):
            across = (((1,), (1,)), ((), ()))
            return lax.dot_general(left, w[:, :half], across, preferred_element_type=F32) + lax.dot_general(
                right, w[:, half:], across, preferred_element_type=F32
            )

        for buf, gate, up in ((eact, eg, eu), (dact, dg, du)):
            g = both(gate)
            buf[c, zd] = (g / (1.0 + jnp.exp(-g)) * both(up)).astype(BF16)
        acts(d, eact, 0).start()
        acts(d, dact, 1).start()

    expert = me // 2

    def send_part(zd, k):
        q = (p + k) % ms
        return remote(sp.at[zd, q], rp.at[zd, p], sp_send.at[zd, k], rp_recv.at[zd, p], (z * ms + q, c))

    def part_arrival(zd, k):
        q = (p + k) % ms
        return remote(sp.at[zd, q], rp.at[zd, q], sp_send.at[zd, k], rp_recv.at[zd, q], (z * ms + q, c))

    def first_leg(zd, k):
        to = flip(p, near)
        return remote(
            sp.at[zd, 3 - p if k == 0 else to], rp.at[zd, k], sp_send.at[zd, k], rp_recv.at[zd, k],
            (z * ms + to, c),
        )

    def next_leg(zd):
        return remote(
            rp.at[zd, 3], rp.at[zd, 2], sp_send.at[zd, 2], rp_recv.at[zd, 2], (z * ms + flip(p, far), c)
        )

    def pass_on(i):
        zd = (z + i) % zs
        first_leg(zd, 0).wait_recv()
        rp[zd, 3] = (sp[zd, flip(p, far)].astype(F32) + rp[zd, 0].astype(F32)).astype(BF16)
        next_leg(zd).start()

    def second(i):
        zd = (z + i) % zs
        for k, buf in enumerate((eact, dact)):
            remote(buf.at[1 - c, zd], buf.at[1 - c, zd], as_send.at[k, zd], as_recv.at[k, zd], other).wait_recv()
        block = pl.ds(zd * ms, ms)
        gate = (
            jnp.sum(rows[0, block].reshape(ms * batch, half).astype(F32) * gline[:, :half], axis=1, keepdims=True)
            + jnp.sum(rows[1, block].reshape(ms * batch, half).astype(F32) * gline[:, half:], axis=1, keepdims=True)
        )
        gate = (1.0 / (1.0 + jnp.exp(-gate))).astype(BF16).astype(F32)
        share = jnp.concatenate([
            column(wtb[zd * ms + q, pl.ds(expert, 1), :], batch) for q in range(ms)
        ], axis=0)
        ew, dw = eact.shape[-1], dact.shape[-1]
        y = share * (
            jnp.dot(eact[0, zd], ed[:ew, :], preferred_element_type=F32)
            + jnp.dot(eact[1, zd], ed[ew:, :], preferred_element_type=F32)
        ) + gate * (
            jnp.dot(dact[0, zd], dd[:dw, :], preferred_element_type=F32)
            + jnp.dot(dact[1, zd], dd[dw:, :], preferred_element_type=F32)
        )
        sp[zd] = y.astype(BF16).reshape(ms, batch, half)
        if quad:
            first_leg(zd, 0).start()
            first_leg(zd, 1).start()
        else:
            loop(1, ms, lambda k: send_part(zd, k).start())

    def gathered(zd):
        if quad:
            first_leg(zd, 1).wait_recv()
            next_leg(zd).wait_recv()
            return sp[zd, p].astype(F32) + rp[zd, 1].astype(F32) + rp[zd, 2].astype(F32)
        loop(1, ms, lambda k: part_arrival(zd, k).wait_recv())
        total = sp[zd, p].astype(F32)
        for k in range(1, ms):
            total = total + rp[zd, (p + k) % ms].astype(F32)
        return total

    def zback(d):
        zd = (z + d) % zs
        return remote(zsend.at[zd], zrecv.at[z], zq_send.at[d], zq_recv.at[z], (zd * ms + p, c))

    def third(d):
        zd = (z + d) % zs
        zsend[zd] = gathered(zd).astype(BF16)
        zback(d).start()

    def stage(low, high, t, body):
        pl.when((t >= low) & (t < high))(body)

    def route_arrivals():
        for load in loads:
            load.wait()
        loop(1, n, lambda k: remote(
            wtb.at[me], wtb.at[(me + k) % n], rsend.at[k], rrecv.at[(me + k) % n], other).wait_recv())

    spread(0)

    def step(t):
        stage(0, zs - 1, t, lambda: spread(t + 1))
        stage(0, zs, t, lambda: collect(t))
        stage(1, 2, t, route_arrivals)
        stage(1, zs + 1, t, lambda: first(t - 1))
        stage(2, zs + 2, t, lambda: second(t - 2))
        if quad:
            stage(3, zs + 3, t, lambda: pass_on(t - 3))
        stage(5, zs + 4, t, lambda: third(t - 4))

    loop(0, zs + 4, step)
    own[...] = gathered(z) + res[:, pl.ds(pl.multiple_of(c * half, half), half)]

    def last(d):
        zd = (z + d) % zs
        remote(zsend.at[zd], zrecv.at[zd], zq_send.at[d], zq_recv.at[zd], other).wait_recv()
        own[...] += zrecv[zd].astype(F32)

    loop(1, zs, last)
    out[...] = own[...].astype(BF16)

    loop(1, n, lambda k: route(k).wait_send())
    loop(1, zs, lambda d: zcopy(d).wait_send())

    def settle(d):
        zd = (z + d) % zs
        if quad:
            plane4(d, 1).wait_send()
            plane4(d, 2).wait_send()
            hop(zd * ms + flip(p, near)).wait_send()
            first_leg(zd, 0).wait_send()
            first_leg(zd, 1).wait_send()
            next_leg(zd).wait_send()
        else:
            loop(1, ms, lambda k: plane(d, k).wait_send())
            loop(1, ms, lambda k: send_part(zd, k).wait_send())
        acts(d, eact, 0).wait_send()
        acts(d, dact, 1).wait_send()

    loop(0, zs, settle)
    loop(1, n, lambda k: forward((me + k) % n).wait_send())
    loop(1, zs, lambda d: zback(d).wait_send())


def per_device(
    n_ep, hidden_in, past_lengths, key_cache, value_cache, attn_gain, w_query, w_key, w_value, lambdas,
    head_gain, w_out, ffn_gain, route_ids, route_weights, expert_gate, expert_up, expert_down,
    gate_vector, dense_gate, dense_up, dense_down,
):
    batch, width = hidden_in.shape
    half = width // 2
    heads = lambdas.shape[0]
    cache_len = key_cache.shape[1]
    middle = HEAD_DIM // 2
    powers = ROPE_BASE ** (-np.arange(middle, dtype=np.float32) / np.float32(middle))
    inverse = jnp.asarray(np.tile(powers.astype(np.float32), 128 // middle)[None, :])
    sem = pltpu.SemaphoreType.DMA
    part, key_new, value_new = pl.pallas_call(
        attention_kernel,
        out_shape=(
            jax.ShapeDtypeStruct((batch, width), BF16),
            jax.ShapeDtypeStruct((batch, 128), BF16),
            jax.ShapeDtypeStruct((batch, 128), BF16),
        ),
        in_specs=[SMEM] * 2 + [VMEM] * 5 + [ANY] * 6,
        out_specs=(VMEM, VMEM, VMEM),
        scratch_shapes=[
            pltpu.VMEM(w_query.shape, BF16),
            pltpu.VMEM(w_key.shape, BF16),
            pltpu.VMEM(w_value.shape, BF16),
            pltpu.VMEM(w_out.shape, BF16),
            pltpu.VMEM((2, GROUP, cache_len, 128), BF16),
            pltpu.VMEM((2, GROUP, cache_len, 128), BF16),
            pltpu.VMEM((batch, heads, 128), F32),
            pltpu.VMEM((batch, heads, 128), F32),
            pltpu.VMEM((batch, 128), F32),
            pltpu.VMEM((batch, 128), F32),
            sem((4,)),
            sem((2, GROUP, cache_len // SPAN, 2)),
        ],
        name="attend",
    )(
        past_lengths, lambdas, past_lengths.reshape(1, -1), inverse, hidden_in,
        attn_gain.reshape(1, -1), head_gain.reshape(1, -1), w_query, w_key, w_value, w_out, key_cache, value_cache,
    )
    experts = n_ep // 2
    zs = 4 if n_ep % 4 == 0 else 1
    ms = n_ep // zs
    expert_w, dense_w = expert_gate.shape[2], dense_gate.shape[1]
    mixed = pl.pallas_call(
        functools.partial(ffn_kernel, n_ep, zs),
        out_shape=jax.ShapeDtypeStruct((batch, half), BF16),
        in_specs=[VMEM] * 6 + [ANY] * 6,
        out_specs=VMEM,
        scratch_shapes=[
            pltpu.VMEM((expert_w, width), BF16),
            pltpu.VMEM((expert_w, width), BF16),
            pltpu.VMEM(expert_down.shape[1:], BF16),
            pltpu.VMEM((dense_w, width), BF16),
            pltpu.VMEM((dense_w, width), BF16),
            pltpu.VMEM(dense_down.shape, BF16),
            pltpu.VMEM((batch, width), BF16),
            pltpu.VMEM((batch, width), F32),
            pltpu.VMEM((2, n_ep, batch, half), BF16),
            pltpu.VMEM((n_ep, experts, 128), F32),
            pltpu.VMEM((2, zs, ms * batch, expert_w), BF16),
            pltpu.VMEM((2, zs, ms * batch, dense_w), BF16),
            pltpu.VMEM((zs, ms, batch, half), BF16),
            pltpu.VMEM((zs, ms, batch, half), BF16),
            pltpu.VMEM((zs, batch, half), BF16),
            pltpu.VMEM((zs, batch, half), BF16),
            pltpu.VMEM((batch, half), F32),
            pltpu.VMEM((1, width), F32),
            sem((6,)), sem((2,)), sem((n_ep,)), sem((n_ep,)), sem((zs,)), sem((zs, ms)), sem((zs,)), sem((n_ep,)),
            sem((n_ep,)), sem((n_ep,)), sem((2, zs)), sem((2, zs)), sem((zs, ms)), sem((zs, ms)),
            sem((zs,)), sem((zs,)),
        ],
        compiler_params=pltpu.CompilerParams(collective_id=0, has_side_effects=True),
        name="feed",
    )(
        part, hidden_in, ffn_gain.reshape(1, -1), route_ids.T, route_weights.T, gate_vector.reshape(-1, 128),
        expert_gate.swapaxes(1, 2), expert_up.swapaxes(1, 2), expert_down,
        dense_gate.T, dense_up.T, dense_down,
    )
    return mixed, key_new, value_new


def solution(mesh):
    return jax.shard_map(
        functools.partial(per_device, mesh.shape["ep"]),
        mesh=mesh,
        in_specs=(
            P("ep", None),
            P("ep"),
            P("ep", None, "tp"),
            P("ep", None, "tp"),
            P(),
            P(None, "tp"),
            P(None, "tp"),
            P(None, "tp"),
            P("tp"),
            P(),
            P("tp", None),
            P(),
            P("ep", None),
            P("ep", None),
            P("ep", None, "tp"),
            P("ep", None, "tp"),
            P("ep", None, "tp"),
            P(),
            P(None, ("ep", "tp")),
            P(None, ("ep", "tp")),
            P("ep", "tp"),
        ),
        out_specs=(P("ep", "tp"), P("ep", "tp"), P("ep", "tp")),
        check_vma=False,
    )
```
